32 devices in a mesh: sp: 4 (over z), fs: 4 (over y, x), tp: 2 (over core).
Axes of the slice: x: 2, y: 2, z: 4, core: 2. Of those that a mesh axis runs over, the one named last changes fastest.
Arguments:
- tokens: bfloat16 [8192, 2048], P(('fs', 'sp')), parts along dimension 0, may hold values from -6 to 6
- norm_gain: bfloat16 [2048], replicated, may hold values from 0.099609375 to 1.8984375
- w_query: bfloat16 [2048, 1024], P('sp', 'tp'), may hold values from -0.15625 to 0.15625
- w_key: bfloat16 [2048, 256], P('sp', 'tp'), may hold values from -0.15625 to 0.15625
- w_value: bfloat16 [2048, 256], P('sp', 'tp'), may hold values from -0.125 to 0.125
- w_glu_value: bfloat16 [2048, 1024], P('sp', 'tp'), may hold values from -0.22097087 to 0.22097087
- w_glu_gate: bfloat16 [2048, 1024], P('sp', 'tp'), may hold values from -0.125 to 0.125
- conv_taps: bfloat16 [31, 1024], P(None, 'tp'), may hold values from -1 to 1
- convolution_norm_gain: bfloat16 [1024], replicated, may hold values from 0.099609375 to 1.8984375
- head_gain: bfloat16 [128], replicated, may hold values from 0.099609375 to 1.8984375
- lam: float32 [8], P('tp'), may hold values from 0.3 to 0.8
- w_out: bfloat16 [2048, 2048], P(None, 'sp'), may hold values from -0.125 to 0.125
Outputs:
- mixed: bfloat16 [8192, 2048], P(('fs', 'sp', 'tp')), parts along dimension 0
- log_totals: float32 [8192, 16], P(('fs', 'sp'), 'tp'), parts along dimension 0
The draws below stay inside these ranges and needn't reach their ends.
There are 4 independent parts, one for each index of `fs`. The reference program is written for one: setup_inputs(seed, part) draws one part's arguments, and reference() takes and returns one part's arrays. A program takes and returns all parts, laid end to end along the dimension named above; an argument that names none is the same for every part. Nothing has to cross between parts.
All inputs are finite; a program needn't handle non-finite values.
Results may differ from the reference program's by a relative error of at most 0.0095.
Values may be sent and summed in bfloat16 or wider, within the bound.
A program may use at most 64 MiB of HBM per device.

```python
import math
import jax
import jax.numpy as jnp
from jax import lax

D = 2048
HEADS = 8
KV_HEADS = 2
QK = 64
VDIM = 128
CONV = 1024
KW = 31
SEQ = 2048


def draw_w_glu_value(key, part):
    first, second = jax.random.split(jax.random.fold_in(key, 41))
    placed = (jnp.arange(CONV, dtype=jnp.float32) + jax.random.uniform(first, (CONV,), jnp.float32)) / CONV
    column_scale = 10.0 ** placed / 4.0
    base = jax.random.truncated_normal(second, -4.0, 4.0, (D, CONV), jnp.float32)
    values = base * column_scale[None, :] * D ** (-0.5)
    return jnp.clip(values, -10.0 * D ** (-0.5), 10.0 * D ** (-0.5)).astype(jnp.bfloat16)


def block_scale(own_key, dims, cuts, low, high):
    def one(axis_at, shards_of):
        draws = jax.random.uniform(jax.random.fold_in(jax.random.fold_in(own_key, 6), axis_at), (shards_of,), jnp.float32, low / len(cuts), high / len(cuts))
        return jnp.repeat(jnp.exp(draws), dims[axis_at] // shards_of).reshape((-1,) + (1,) * (len(dims) - axis_at - 1))

    level = one(*cuts[0])
    for cut in cuts[1:]:
        level = level * one(*cut)
    return level


def bell_draw(key, extent, scale, limit, cuts=(), kind=jnp.bfloat16):
    entries = jax.random.normal(key, extent, jnp.float32) * scale
    if len(cuts) > 0:
        entries = block_scale(key, extent, cuts, -0.22, 0.18) * entries
    return jnp.clip(entries, min=-limit, max=limit).astype(kind)


def setup_inputs(seed: int = 0, part: int = 0) -> dict:
    streams_of = jax.random.split(jax.random.key(seed), 13)
    part_keys = jax.random.split(jax.random.fold_in(streams_of[12], part), 13)
    return {
        "tokens": bell_draw(part_keys[0], (SEQ, D), 1.0, 6.0, ((0, 4),)),
        "norm_gain": jnp.clip(1.0 + 0.18 * jax.random.normal(streams_of[1], (D,), jnp.float32), 0.099609375, 1.8984375).astype(jnp.bfloat16),
        "w_query": bell_draw(streams_of[2], (D, HEADS * 2 * QK), (D * 2 // 3) ** -0.5, 0.15625, ((0, 4), (1, 2))),
        "w_key": bell_draw(streams_of[3], (D, KV_HEADS * 2 * QK), (D * 2 // 3) ** -0.5, 0.15625, ((0, 4), (1, 2))),
        "w_value": bell_draw(streams_of[4], (D, KV_HEADS * VDIM), D ** -0.5, 0.125, ((0, 4), (1, 2))),
        "w_glu_value": draw_w_glu_value(jax.random.fold_in(streams_of[12], 71), part),
        "w_glu_gate": bell_draw(streams_of[6], (D, CONV), D ** -0.5, 0.125, ((0, 4), (1, 2))),
        "conv_taps": bell_draw(streams_of[7], (KW, CONV), KW ** -0.5, 1.0, ((1, 2),)),
        "convolution_norm_gain": jnp.clip(1.0 + 0.18 * jax.random.normal(streams_of[8], (CONV,), jnp.float32), 0.099609375, 1.8984375).astype(jnp.bfloat16),
        "head_gain": jnp.clip(1.0 + 0.18 * jax.random.normal(streams_of[9], (VDIM,), jnp.float32), 0.099609375, 1.8984375).astype(jnp.bfloat16),
        "lam": jnp.clip(0.3 + 0.5 * jax.random.uniform(streams_of[10], (HEADS,), jnp.float32) ** block_scale(streams_of[10], (HEADS,), ((0, 2),), -0.2, 0.2), 0.3, 0.8),
        "w_out": bell_draw(streams_of[11], (HEADS * VDIM + CONV, D), (HEADS * VDIM + CONV) ** -0.5, 0.125, ((1, 4),)),
    }


def reference(tokens, norm_gain, w_query, w_key, w_value, w_glu_value, w_glu_gate, conv_taps, convolution_norm_gain, head_gain, lam, w_out):
    length = tokens.shape[0]
    eps = 1e-06
    tok32 = tokens.astype(jnp.float32)
    normalized_rows = (tok32 * lax.rsqrt(lax.optimization_barrier(jnp.mean(tok32 * tok32, axis=-1, keepdims=True)) + eps) * norm_gain.astype(jnp.float32)).astype(jnp.bfloat16)
    queries = jnp.dot(normalized_rows, w_query, preferred_element_type=jnp.float32).astype(jnp.bfloat16)
    keys = jnp.dot(normalized_rows, w_key, preferred_element_type=jnp.float32).astype(jnp.bfloat16)
    values = jnp.dot(normalized_rows, w_value, preferred_element_type=jnp.float32).astype(jnp.bfloat16)
    glu_val = jnp.dot(normalized_rows, w_glu_value, preferred_element_type=jnp.float32)
    glu_gate = jnp.dot(normalized_rows, w_glu_gate, preferred_element_type=jnp.float32)
    gated = (glu_val * jax.nn.sigmoid(glu_gate)).astype(jnp.bfloat16)
    padded = jnp.concatenate([jnp.zeros((KW - 1, CONV), jnp.bfloat16), gated], axis=0)
    conv = jnp.zeros((length, CONV), jnp.float32)
    for tap in range(KW):
        conv = conv + conv_taps[tap].astype(jnp.float32) * padded[tap:tap + length].astype(jnp.float32)
    conv = conv.astype(jnp.bfloat16).astype(jnp.float32)
    conv_act = jax.nn.silu(conv * lax.rsqrt(lax.optimization_barrier(jnp.mean(conv * conv, axis=-1, keepdims=True)) + eps) * convolution_norm_gain.astype(jnp.float32)).astype(jnp.bfloat16)
    group = HEADS // KV_HEADS
    key_all = keys.astype(jnp.float32).reshape(length, KV_HEADS, 2, QK)
    value_rows_full = values.astype(jnp.float32).reshape(length, KV_HEADS, VDIM)
    block = math.gcd(length, 512)
    query_blocks = queries.reshape(length // block, block, KV_HEADS, group, 2, QK)
    key_pos = jnp.arange(length, dtype=jnp.int32)

    def one_block(item):
        query_block, index = item
        qfloat = query_block.astype(jnp.float32)
        score = jnp.einsum('tkgmd,nkmd->tkgmn', qfloat, key_all) * QK ** (-0.5)
        query_pos = index * block + jnp.arange(block, dtype=jnp.int32)
        allowed = key_pos[None, None, None, None, :] <= query_pos[:, None, None, None, None]
        weight = jnp.where(allowed, jnp.exp(score), 0.0)
        total = lax.optimization_barrier(jnp.sum(weight, axis=-1))
        rounded_values = weight.astype(jnp.bfloat16).astype(jnp.float32)
        running_total = jnp.einsum('doejz,zow->doejw', rounded_values, value_rows_full)
        return (running_total, total)
    running_total, total = lax.map(one_block, (query_blocks, jnp.arange(length // block, dtype=jnp.int32)))
    running_total = running_total.reshape(length, HEADS, 2, VDIM)
    total = total.reshape(length, HEADS, 2)
    lam32 = lam.astype(jnp.float32)
    diff = running_total[:, :, 0] / total[:, :, 0, None] - lam32[None, :, None] * running_total[:, :, 1] / total[:, :, 1, None]
    att_out = diff * lax.rsqrt(lax.optimization_barrier(jnp.mean(diff * diff, axis=-1, keepdims=True)) + eps) * head_gain.astype(jnp.float32)
    att_out = att_out.astype(jnp.bfloat16).reshape(length, HEADS * VDIM)
    log_totals = jnp.log(total).reshape(length, HEADS * 2)
    both = jnp.concatenate([att_out, conv_act], axis=1)
    mixed = jnp.dot(both, w_out, preferred_element_type=jnp.float32).astype(jnp.bfloat16)
    return (mixed, log_totals)
```

```python
import functools
import math

import jax
import jax.numpy as jnp
from jax import lax
from jax.experimental import pallas as pl
from jax.experimental.pallas import tpu as pltpu
from jax.sharding import PartitionSpec as P

QK = 64
VDIM = 128
EPS = 1e-06
MESH = pl.DeviceIdType.MESH
BF = jnp.bfloat16
F32 = jnp.float32
LANES = 128
RIM = 32


def kernel(
    n,
    conv_total,
    tok_h,
    gain_r,
    wq_h,
    wk_h,
    wv_h,
    wgv_h,
    wgg_h,
    taps_r,
    cgain_r,
    hgain_r,
    lam_r,
    wo_h,
    mixed_r,
    log_r,
    tok,
    normed,
    ga,
    gb,
    gc,
    q2,
    kbuf,
    vbuf,
    acc,
    gated,
    rim,
    pad,
    conv,
    sq_own,
    sq_in,
    both,
    part_out,
    part_in,
    keep,
    loc,
    zs,
    zr,
    xs,
    xr,
    ys,
    yr,
    hxs,
    hxr,
    hys,
    hyr,
    kvs,
    kvr,
    rims,
    sqs,
    ps,
    pr,
):
    s = lax.axis_index("sp")
    f = lax.axis_index("fs")
    t = lax.axis_index("tp")
    fx = f + 1 - 2 * (f % 2)
    fy = (f + 2) % 4
    left = {"sp": s - 1, "fs": f, "tp": t}
    right = {"sp": s + 1, "fs": f, "tp": t}
    xdev = {"sp": s, "fs": fx, "tp": t}
    ydev = {"sp": s, "fs": fy, "tp": t}
    mate = {"sp": s, "fs": f, "tp": 1 - t}
    rows, width = tok.shape
    heads = lam_r.shape[0]
    chans = gated.shape[1]
    qcols = wq_h.shape[1]
    half = rows // 2
    groups = (ga, gb, gc)
    has_left = s > 0
    has_right = s < n - 1

    d_rows = wq_h.shape[0]
    att_rows = heads * VDIM
    locals_ = [
        (wq_h, ga.at[s, :, pl.ds(0, qcols)]),
        (wk_h, ga.at[s, :, pl.ds(qcols, LANES)]),
        (wv_h, ga.at[s, :, pl.ds(qcols + LANES, LANES)]),
        (tok_h, tok),
        (wgv_h, gb.at[s, :, pl.ds(0, chans)]),
        (wgg_h, gb.at[s, :, pl.ds(chans, chans)]),
        (wo_h.at[pl.ds(t * att_rows, att_rows), :], gc.at[s, pl.ds(0, att_rows), :]),
        (
            wo_h.at[pl.ds(2 * att_rows + t * chans, chans), :],
            gc.at[s, pl.ds(att_rows, chans), :],
        ),
    ]
    copies = [pltpu.make_async_copy(a, b, loc.at[i]) for i, (a, b) in enumerate(locals_)]
    for c in copies:
        c.start()

    bar = pltpu.get_barrier_semaphore()
    for dev in (xdev, ydev, mate):
        pl.semaphore_signal(bar, 1, device_id=dev, device_id_type=MESH)

    @pl.when(has_left)
    def _():
        pl.semaphore_signal(bar, 1, device_id=left, device_id_type=MESH)

    @pl.when(has_right)
    def _():
        pl.semaphore_signal(bar, 1, device_id=right, device_id_type=MESH)

    pl.semaphore_wait(bar, 3 + jnp.where(has_left, 1, 0) + jnp.where(has_right, 1, 0))

    def chunk(g, o, q, part=None):
        buf = groups[g]
        size = buf.shape[1] // 4
        if part is None:
            return buf.at[o, pl.ds(pl.multiple_of(q * size, size), size), :]
        size = size // 2
        return buf.at[o, pl.ds(pl.multiple_of((q * 2 + part) * size, size), size), :]

    def zcopy(g, o, right_way):
        c = chunk(g, o, f)
        return pltpu.make_async_remote_copy(
            c,
            c,
            zs.at[g, 0 if right_way else 1, o],
            zr.at[g, o],
            device_id=right if right_way else left,
            device_id_type=MESH,
        )

    def xcopy(g, o, q):
        c = chunk(g, o, q)
        return pltpu.make_async_remote_copy(
            c, c, xs.at[g, o], xr.at[g, o], device_id=xdev, device_id_type=MESH
        )

    def ycopy(g, o, q):
        c = chunk(g, o, q)
        return pltpu.make_async_remote_copy(
            c, c, ys.at[g, o], yr.at[g, o], device_id=ydev, device_id_type=MESH
        )

    def hxcopy(g, o, q):
        c = chunk(g, o, q, 0)
        return pltpu.make_async_remote_copy(
            c, c, hxs.at[g, o], hxr.at[g, o], device_id=xdev, device_id_type=MESH
        )

    def hycopy(g, o, q):
        c = chunk(g, o, q, 1)
        return pltpu.make_async_remote_copy(
            c, c, hys.at[g, o], hyr.at[g, o], device_id=ydev, device_id_type=MESH
        )

    fd = 3 - f

    def sides(k, fn):
        @pl.when(s >= k)
        def _():
            fn(s - k, True)

        @pl.when(s + k < n)
        def _():
            fn(s + k, False)

    def own_send(g):
        @pl.when(has_right)
        def _():
            zcopy(g, s, True).start()

        @pl.when(has_left)
        def _():
            zcopy(g, s, False).start()

    def stage1(g, k):
        def go(o, right_way):
            zcopy(g, o, right_way).wait_recv()
            xcopy(g, o, f).start()
            ycopy(g, o, f).start()

            @pl.when(has_right if right_way else has_left)
            def _():
                zcopy(g, o, right_way).start()

        sides(k, go)

    def stage2(g, k):
        def go(o, right_way):
            xcopy(g, o, fx).wait_recv()
            hycopy(g, o, fx).start()
            ycopy(g, o, fy).wait_recv()
            hxcopy(g, o, fy).start()

        sides(k, go)

    def stage3(g, k):
        def go(o, right_way):
            hxcopy(g, o, fd).wait_recv()
            hycopy(g, o, fd).wait_recv()

        sides(k, go)

    def drain(g):
        own = zcopy(g, s, True)

        @pl.when(has_right)
        def _():
            own.wait_send()

        @pl.when(has_left)
        def _():
            zcopy(g, s, False).wait_send()

        for k in range(1, n):

            def go(o, right_way):
                xcopy(g, o, f).wait_send()
                ycopy(g, o, f).wait_send()
                hycopy(g, o, fx).wait_send()
                hxcopy(g, o, fy).wait_send()

                @pl.when(has_right if right_way else has_left)
                def _():
                    zcopy(g, o, right_way).wait_send()

            sides(k, go)

    def kvcopy(o):
        return [
            pltpu.make_async_remote_copy(
                b.at[o], b.at[o], kvs.at[i, o], kvr.at[i, o], device_id=right, device_id_type=MESH
            )
            for i, b in enumerate((kbuf, vbuf))
        ]

    def kv_take(k):
        @pl.when(s >= k)
        def _():
            for c in kvcopy(s - k):
                c.wait_recv()

            @pl.when(has_right)
            def _():
                for c in kvcopy(s - k):
                    c.start()

    tall = min(256, rows)
    per_head = 2 * rows // tall

    def attend(o, diagonal):
        vx = jnp.concatenate([vbuf[o], jnp.ones((rows, VDIM), BF)], axis=1)
        kx = kbuf[o]

        def step(i, carry):
            h = i // per_head
            at = pl.multiple_of((i % per_head) * tall, tall)
            score = lax.dot_general(
                q2[h, pl.ds(at, tall), :],
                kx,
                (((1,), (1,)), ((), ())),
                preferred_element_type=F32,
            )
            w = jnp.exp2(score * (QK**-0.5 * math.log2(math.e)))
            if diagonal:
                pos = (at % rows) + lax.broadcasted_iota(jnp.int32, w.shape, 0)
                w = jnp.where(lax.broadcasted_iota(jnp.int32, w.shape, 1) <= pos, w, 0.0)
            pv = jnp.dot(w.astype(BF), vx, preferred_element_type=F32)
            if diagonal:
                acc[h, pl.ds(at, tall), :] = pv
            else:
                acc[h, pl.ds(at, tall), :] += pv
            return carry

        lax.fori_loop(0, heads * per_head, step, 0, unroll=2)

    def attend_back(k):
        @pl.when(s >= k)
        def _():
            attend(s - k, False)

    for c in copies[:3]:
        c.wait()
    own_send(0)
    copies[3].wait()

    def norm_step(i, carry):
        at = pl.ds(pl.multiple_of(i * 32, 32), 32)
        x = tok[at, :].astype(F32)
        r = lax.rsqrt(jnp.mean(x * x, axis=-1, keepdims=True) + EPS)
        normed[at, :] = (x * r * gain_r[...].astype(F32)).astype(BF)
        return carry

    lax.fori_loop(0, rows // 32, norm_step, 0)
    for c in copies[4:]:
        c.wait()

    for k in range(1, n):
        stage1(0, k)
        if k == 1:
            own_send(1)
        if k > 1:
            stage2(0, k - 1)
    if n > 1:
        stage2(0, n - 1)
        stage1(1, 1)
        own_send(2)
    for k in range(1, n):
        stage3(0, k)

    lane = lax.broadcasted_iota(jnp.int32, (rows, LANES), 1)

    kv = jnp.dot(
        normed[...],
        ga[:, :, qcols : qcols + 2 * LANES].reshape(width, 2 * LANES),
        preferred_element_type=F32,
    ).astype(BF)
    kbuf[s] = kv[:, :LANES]
    vbuf[s] = kv[:, LANES:]

    @pl.when(has_right)
    def _():
        for c in kvcopy(s):
            c.start()

    def q_step(h, carry):
        cols = pl.ds(pl.multiple_of(h * 2 * LANES, 2 * LANES), 2 * LANES)
        q = jnp.dot(normed[...], ga[:, :, cols].reshape(width, 2 * LANES), preferred_element_type=F32)
        for e in range(2):
            one = q[:, e * LANES : (e + 1) * LANES]
            q2[2 * h + e, :rows, :] = jnp.where(lane < QK, one, 0.0).astype(BF)
            q2[2 * h + e, rows:, :] = jnp.where(lane >= QK, one, 0.0).astype(BF)
        return carry

    lax.fori_loop(0, heads // 2, q_step, 0)

    if n > 2:
        stage1(1, 2)
    if n > 1:
        stage2(1, 1)
    attend(s, True)
    for k in range(3, n):
        stage1(1, k)
        stage2(1, k - 1)
    if n > 1:
        kv_take(1)
    if n > 2:
        stage2(1, n - 1)
    if n > 1:
        attend_back(1)
        stage1(2, 1)
    for k in range(1, n):
        stage3(1, k)

    def glu_step(i, carry):
        at = pl.multiple_of(i * 2 * LANES, 2 * LANES)
        cols = pl.ds(at, 2 * LANES)
        cols_gate = pl.ds(pl.multiple_of(chans + at, 2 * LANES), 2 * LANES)
        val = jnp.dot(normed[...], gb[:, :, cols].reshape(width, 2 * LANES), preferred_element_type=F32)
        gate = jnp.dot(
            normed[...], gb[:, :, cols_gate].reshape(width, 2 * LANES), preferred_element_type=F32
        )
        g = (val * jax.nn.sigmoid(gate)).astype(BF)
        gated[:, cols] = g
        pad[RIM:, cols] = g.astype(F32)
        return carry

    lax.fori_loop(0, chans // (2 * LANES), glu_step, 0)

    rim_copy = pltpu.make_async_remote_copy(
        gated.at[pl.ds(rows - RIM, RIM), :],
        rim,
        rims.at[0],
        rims.at[1],
        device_id=right,
        device_id_type=MESH,
    )

    @pl.when(has_right)
    def _():
        rim_copy.start()

    for k in range(2, n):
        stage1(2, k)
        stage2(2, k - 1)
        kv_take(k)
        attend_back(k)
    if n > 1:
        stage2(2, n - 1)

    @pl.when(has_left)
    def _():
        rim_copy.wait_recv()
        pad[:RIM, :] = rim[...].astype(F32)

    @pl.when(s == 0)
    def _():
        pad[:RIM, :] = jnp.zeros((RIM, chans), F32)

    taps = taps_r.shape[0]
    shift = RIM - (taps - 1)
    tile = min(128, rows)

    def conv_step(i, carry):
        cols = pl.ds(pl.multiple_of(i * LANES, LANES), LANES)
        for r in range(0, rows, tile):
            total = jnp.zeros((tile, LANES), F32)
            for j in range(taps):
                total = total + taps_r[j : j + 1, cols].astype(F32) * pad[
                    r + shift + j : r + shift + j + tile, cols
                ]
            conv[r : r + tile, cols] = total.astype(BF).astype(F32)
        return carry

    lax.fori_loop(0, chans // LANES, conv_step, 0)
    cv = conv[...]
    sq_own[...] = jnp.broadcast_to(jnp.sum(cv * cv, axis=-1, keepdims=True), (rows, LANES))
    sq_copy = pltpu.make_async_remote_copy(
        sq_own, sq_in, sqs.at[0], sqs.at[1], device_id=mate, device_id_type=MESH
    )
    sq_copy.start()

    def head_rows(i, carry):
        at = pl.multiple_of(i * tile, tile)
        ids = lax.broadcasted_iota(jnp.int32, (tile, LANES), 1)
        logs = jnp.zeros((tile, LANES), F32)
        for h in range(heads):
            a0 = acc[h, pl.ds(at, tile), :]
            a1 = acc[h, pl.ds(pl.multiple_of(rows + at, tile), tile), :]
            t0, t1 = a0[:, VDIM:], a1[:, VDIM:]
            diff = a0[:, :VDIM] / t0 - lam_r[h] * (a1[:, :VDIM] / t1)
            out = (
                diff
                * lax.rsqrt(jnp.mean(diff * diff, axis=-1, keepdims=True) + EPS)
                * hgain_r[...].astype(F32)
            )
            both[pl.ds(at, tile), h * VDIM : (h + 1) * VDIM] = out.astype(BF)
            logs = jnp.where(ids == 2 * h, jnp.log(t0), logs)
            logs = jnp.where(ids == 2 * h + 1, jnp.log(t1), logs)
        log_r[pl.ds(at, tile), :] = logs[:, : 2 * heads]
        return carry

    lax.fori_loop(0, rows // tile, head_rows, 0)

    sq_copy.wait()
    inv = lax.rsqrt((sq_own[:, :1] + sq_in[:, :1]) / conv_total + EPS)
    cgain = cgain_r[:, pl.ds(pl.multiple_of(t * chans, LANES), chans)].astype(F32)
    both[:, att_rows:] = jax.nn.silu(conv[...] * inv * cgain).astype(BF)

    def pcopy(o):
        return pltpu.make_async_remote_copy(
            part_out.at[o], part_in.at[o], ps.at[o], pr.at[o], device_id=mate, device_id_type=MESH
        )

    ocols = gc.shape[2]
    mine = pl.ds(pl.multiple_of(t * half, half), half)
    other = pl.ds(pl.multiple_of((1 - t) * half, half), half)

    def out_block(o, _):
        part_out[o] = jnp.dot(both[other, :], gc[o], preferred_element_type=F32).astype(BF)
        pcopy(o).start()
        own = jnp.dot(both[mine, :], gc[o], preferred_element_type=F32)
        keep[o] = own

    out_block(s, None)
    for k in range(1, n):
        stage3(2, k)
        sides(k, out_block)

    def finish(o, carry):
        pcopy(o).wait_recv()
        pcopy(o).wait_send()
        mixed_r[:, pl.ds(pl.multiple_of(o * ocols, ocols), ocols)] = (
            keep[o] + part_in[o].astype(F32)
        ).astype(BF)
        return carry

    lax.fori_loop(0, n, finish, 0)

    for g in range(3):
        drain(g)

    @pl.when(has_right)
    def _():
        rim_copy.wait_send()
        for c in kvcopy(s):
            c.wait_send()

    for k in range(1, n):

        @pl.when((s >= k) & has_right)
        def _():
            for c in kvcopy(s - k):
                c.wait_send()


def body(n, conv_total, tokens, norm_gain, w_query, w_key, w_value, w_gv, w_gg, taps, cgain, hgain, lam, w_out):
    rows, width = tokens.shape
    heads = lam.shape[0]
    chans = w_gv.shape[1]
    qcols = w_query.shape[1]
    wrows = w_query.shape[0]
    ocols = w_out.shape[1]
    half = rows // 2
    any_ = pl.BlockSpec(memory_space=pl.ANY)
    vm = pl.BlockSpec(memory_space=pltpu.VMEM)
    sm = pl.BlockSpec(memory_space=pltpu.SMEM)
    dma = pltpu.SemaphoreType.DMA
    v = pltpu.VMEM
    return pl.pallas_call(
        functools.partial(kernel, n, conv_total),
        out_shape=(
            jax.ShapeDtypeStruct((half, width), BF),
            jax.ShapeDtypeStruct((rows, 2 * heads), F32),
        ),
        in_specs=[any_, vm, any_, any_, any_, any_, any_, vm, vm, vm, sm, any_],
        out_specs=(vm, vm),
        scratch_shapes=[
            v((rows, width), BF),
            v((rows, width), BF),
            v((n, wrows, qcols + 2 * LANES), BF),
            v((n, wrows, 2 * chans), BF),
            v((n, heads * VDIM + chans, ocols), BF),
            v((heads, 2 * rows, LANES), BF),
            v((n, rows, LANES), BF),
            v((n, rows, LANES), BF),
            v((heads, 2 * rows, 2 * VDIM), F32),
            v((rows, chans), BF),
            v((RIM, chans), BF),
            v((rows + RIM, chans), F32),
            v((rows, chans), F32),
            v((rows, LANES), F32),
            v((rows, LANES), F32),
            v((rows, heads * VDIM + chans), BF),
            v((n, half, ocols), BF),
            v((n, half, ocols), BF),
            v((n, half, ocols), F32),
            dma((8,)),
            dma((3, 2, n)),
            dma((3, n)),
            dma((3, n)),
            dma((3, n)),
            dma((3, n)),
            dma((3, n)),
            dma((3, n)),
            dma((3, n)),
            dma((3, n)),
            dma((3, n)),
            dma((2, n)),
            dma((2, n)),
            dma((2,)),
            dma((2,)),
            dma((n,)),
            dma((n,)),
        ],
        compiler_params=pltpu.CompilerParams(
            collective_id=0, has_side_effects=True, vmem_limit_bytes=60 * 1024 * 1024
        ),
    )(
        tokens,
        norm_gain.reshape(1, -1),
        w_query,
        w_key,
        w_value,
        w_gv,
        w_gg,
        taps,
        cgain.reshape(1, -1),
        hgain.reshape(1, -1),
        lam,
        w_out,
    )


def solution(mesh):
    n = mesh.shape["sp"]

    def run(*args):
        return body(n, args[8].shape[0], *args)

    return jax.shard_map(
        run,
        mesh=mesh,
        in_specs=(
            P(("fs", "sp"), None),
            P(),
            P("sp", "tp"),
            P("sp", "tp"),
            P("sp", "tp"),
            P("sp", "tp"),
            P("sp", "tp"),
            P(None, "tp"),
            P(),
            P(),
            P("tp"),
            P(None, "sp"),
        ),
        out_specs=(P(("fs", "sp", "tp"), None), P(("fs", "sp"), "tp")),
        check_vma=False,
    )
```

```python
import functools
import math

import jax
import jax.numpy as jnp
from jax import lax
from jax.experimental import pallas as pl
from jax.experimental.pallas import tpu as pltpu
from jax.sharding import PartitionSpec as P

QK = 64
VDIM = 128
EPS = 1e-06
MESH = pl.DeviceIdType.MESH
BF = jnp.bfloat16
F32 = jnp.float32
LANES = 128
RIM = 32


def kernel(
    n,
    conv_total,
    tok_h,
    gain_r,
    wq_h,
    wk_h,
    wv_h,
    wgv_h,
    wgg_h,
    taps_r,
    cgain_r,
    hgain_r,
    lam_r,
    wo_h,
    mixed_r,
    log_r,
    tok,
    normed,
    gkv,
    gq,
    gb,
    gc,
    q2,
    kbuf,
    vbuf,
    acc,
    gated,
    rim,
    pad,
    conv,
    sq_own,
    sq_in,
    both,
    part_out,
    part_in,
    keep,
    loc,
    zs,
    zr,
    xs,
    xr,
    ys,
    yr,
    hxs,
    hxr,
    hys,
    hyr,
    kvs,
    kvr,
    rims,
    sqs,
    ps,
    pr,
):
    s = lax.axis_index("sp")
    f = lax.axis_index("fs")
    t = lax.axis_index("tp")
    fx = f + 1 - 2 * (f % 2)
    fy = (f + 2) % 4
    left = {"sp": s - 1, "fs": f, "tp": t}
    right = {"sp": s + 1, "fs": f, "tp": t}
    xdev = {"sp": s, "fs": fx, "tp": t}
    ydev = {"sp": s, "fs": fy, "tp": t}
    mate = {"sp": s, "fs": f, "tp": 1 - t}
    rows, width = tok.shape
    heads = lam_r.shape[0]
    chans = gated.shape[1]
    qcols = wq_h.shape[1]
    half = rows // 2
    groups = (gkv, gq, gb, gc)
    has_left = s > 0
    has_right = s < n - 1

    d_rows = wq_h.shape[0]
    att_rows = heads * VDIM
    locals_ = [
        (wk_h, gkv.at[s, :, pl.ds(0, LANES)]),
        (wv_h, gkv.at[s, :, pl.ds(LANES, LANES)]),
        (wq_h, gq.at[s]),
        (tok_h, tok),
        (wgv_h, gb.at[s, :, pl.ds(0, chans)]),
        (wgg_h, gb.at[s, :, pl.ds(chans, chans)]),
        (wo_h.at[pl.ds(t * att_rows, att_rows), :], gc.at[s, pl.ds(0, att_rows), :]),
        (
            wo_h.at[pl.ds(2 * att_rows + t * chans, chans), :],
            gc.at[s, pl.ds(att_rows, chans), :],
        ),
    ]
    copies = [pltpu.make_async_copy(a, b, loc.at[i]) for i, (a, b) in enumerate(locals_)]
    for c in copies:
        c.start()

    bar = pltpu.get_barrier_semaphore()
    for dev in (xdev, ydev, mate):
        pl.semaphore_signal(bar, 1, device_id=dev, device_id_type=MESH)

    @pl.when(has_left)
    def _():
        pl.semaphore_signal(bar, 1, device_id=left, device_id_type=MESH)

    @pl.when(has_right)
    def _():
        pl.semaphore_signal(bar, 1, device_id=right, device_id_type=MESH)

    pl.semaphore_wait(bar, 3 + jnp.where(has_left, 1, 0) + jnp.where(has_right, 1, 0))

    def chunk(g, o, q, part=None):
        buf = groups[g]
        size = buf.shape[1] // 4
        if part is None:
            return buf.at[o, pl.ds(pl.multiple_of(q * size, size), size), :]
        size = size // 2
        return buf.at[o, pl.ds(pl.multiple_of((q * 2 + part) * size, size), size), :]

    def zcopy(g, o, right_way):
        c = chunk(g, o, f)
        return pltpu.make_async_remote_copy(
            c,
            c,
            zs.at[g, 0 if right_way else 1, o],
            zr.at[g, o],
            device_id=right if right_way else left,
            device_id_type=MESH,
        )

    def xcopy(g, o, q):
        c = chunk(g, o, q)
        return pltpu.make_async_remote_copy(
            c, c, xs.at[g, o], xr.at[g, o], device_id=xdev, device_id_type=MESH
        )

    def ycopy(g, o, q):
        c = chunk(g, o, q)
        return pltpu.make_async_remote_copy(
            c, c, ys.at[g, o], yr.at[g, o], device_id=ydev, device_id_type=MESH
        )

    def hxcopy(g, o, q):
        c = chunk(g, o, q, 0)
        return pltpu.make_async_remote_copy(
            c, c, hxs.at[g, o], hxr.at[g, o], device_id=xdev, device_id_type=MESH
        )

    def hycopy(g, o, q):
        c = chunk(g, o, q, 1)
        return pltpu.make_async_remote_copy(
            c, c, hys.at[g, o], hyr.at[g, o], device_id=ydev, device_id_type=MESH
        )

    fd = 3 - f

    def sides(k, fn):
        @pl.when(s >= k)
        def _():
            fn(s - k, True)

        @pl.when(s + k < n)
        def _():
            fn(s + k, False)

    def own_send(g):
        @pl.when(has_right)
        def _():
            zcopy(g, s, True).start()

        @pl.when(has_left)
        def _():
            zcopy(g, s, False).start()

    def stage1(g, k):
        def go(o, right_way):
            zcopy(g, o, right_way).wait_recv()
            xcopy(g, o, f).start()
            ycopy(g, o, f).start()

            @pl.when(has_right if right_way else has_left)
            def _():
                zcopy(g, o, right_way).start()

        sides(k, go)

    def stage2(g, k):
        def go(o, right_way):
            xcopy(g, o, fx).wait_recv()
            hycopy(g, o, fx).start()
            ycopy(g, o, fy).wait_recv()
            hxcopy(g, o, fy).start()

        sides(k, go)

    def stage3(g, k):
        def go(o, right_way):
            hxcopy(g, o, fd).wait_recv()
            hycopy(g, o, fd).wait_recv()

        sides(k, go)

    def drain(g):
        own = zcopy(g, s, True)

        @pl.when(has_right)
        def _():
            own.wait_send()

        @pl.when(has_left)
        def _():
            zcopy(g, s, False).wait_send()

        for k in range(1, n):

            def go(o, right_way):
                xcopy(g, o, f).wait_send()
                ycopy(g, o, f).wait_send()
                hycopy(g, o, fx).wait_send()
                hxcopy(g, o, fy).wait_send()

                @pl.when(has_right if right_way else has_left)
                def _():
                    zcopy(g, o, right_way).wait_send()

            sides(k, go)

    def kvcopy(o):
        return [
            pltpu.make_async_remote_copy(
                b.at[o], b.at[o], kvs.at[i, o], kvr.at[i, o], device_id=right, device_id_type=MESH
            )
            for i, b in enumerate((kbuf, vbuf))
        ]

    def kv_take(k):
        @pl.when(s >= k)
        def _():
            for c in kvcopy(s - k):
                c.wait_recv()

            @pl.when(has_right)
            def _():
                for c in kvcopy(s - k):
                    c.start()

    tall = min(256, rows)
    per_head = 2 * rows // tall

    def attend(o, diagonal):
        vx = jnp.concatenate([vbuf[o], jnp.ones((rows, VDIM), BF)], axis=1)
        kx = kbuf[o]

        def step(i, carry):
            h = i // per_head
            at = pl.multiple_of((i % per_head) * tall, tall)
            score = lax.dot_general(
                q2[h, pl.ds(at, tall), :],
                kx,
                (((1,), (1,)), ((), ())),
                preferred_element_type=F32,
            )
            w = jnp.exp2(score * (QK**-0.5 * math.log2(math.e)))
            if diagonal:
                pos = (at % rows) + lax.broadcasted_iota(jnp.int32, w.shape, 0)
                w = jnp.where(lax.broadcasted_iota(jnp.int32, w.shape, 1) <= pos, w, 0.0)
            pv = jnp.dot(w.astype(BF), vx, preferred_element_type=F32)
            if diagonal:
                acc[h, pl.ds(at, tall), :] = pv
            else:
                acc[h, pl.ds(at, tall), :] += pv
            return carry

        lax.fori_loop(0, heads * per_head, step, 0, unroll=2)

    def attend_back(k):
        @pl.when(s >= k)
        def _():
            attend(s - k, False)

    items = [(g, k) for g in range(4) for k in range(1, n)]
    per = n - 1
    state = {"at": 0}

    def advance(to):
        to = min(to, len(items))
        for i in range(state["at"], to):
            stage1(*items[i])
            if i == per:
                own_send(2)
            if i == 2 * per:
                own_send(3)
            if i > 0:
                stage2(*items[i - 1])
        state["at"] = max(state["at"], to)

    def arrived(g):
        for k in range(1, n):
            stage3(g, k)

    for c in copies[:2]:
        c.wait()
    own_send(0)
    copies[2].wait()
    own_send(1)
    copies[3].wait()

    gain = gain_r[...].reshape(1, width).astype(F32)

    def norm_step(i, carry):
        at = pl.ds(pl.multiple_of(i * 32, 32), 32)
        x = tok[at, :].astype(F32)
        r = lax.rsqrt(jnp.mean(x * x, axis=-1, keepdims=True) + EPS)
        normed[at, :] = (x * r * gain).astype(BF)
        return carry

    def norm_rows(lo, hi):
        lax.fori_loop(lo, hi, norm_step, 0)

    steps = rows // 32
    norm_rows(0, steps // 2)
    advance(1)
    norm_rows(steps // 2, steps)
    for c in copies[4:]:
        c.wait()
    advance(per + 2)
    arrived(0)

    lane = lax.broadcasted_iota(jnp.int32, (rows, LANES), 1)

    kv = jnp.dot(
        normed[...],
        gkv[...].reshape(width, 2 * LANES),
        preferred_element_type=F32,
    ).astype(BF)
    kbuf[s] = kv[:, :LANES]
    vbuf[s] = kv[:, LANES:]

    @pl.when(has_right)
    def _():
        for c in kvcopy(s):
            c.start()

    advance(2 * per + 2)
    arrived(1)

    def q_step(h, carry):
        cols = pl.ds(pl.multiple_of(h * 2 * LANES, 2 * LANES), 2 * LANES)
        q = jnp.dot(normed[...], gq[:, :, cols].reshape(width, 2 * LANES), preferred_element_type=F32)
        for e in range(2):
            one = q[:, e * LANES : (e + 1) * LANES]
            q2[2 * h + e, :rows, :] = jnp.where(lane < QK, one, 0.0).astype(BF)
            q2[2 * h + e, rows:, :] = jnp.where(lane >= QK, one, 0.0).astype(BF)
        return carry

    lax.fori_loop(0, heads // 2, q_step, 0)

    attend(s, True)
    advance(3 * per + 1)
    kv_take(1)
    attend_back(1)
    advance(3 * per + 2)
    arrived(2)

    def glu_step(i, carry):
        at = pl.multiple_of(i * 2 * LANES, 2 * LANES)
        cols = pl.ds(at, 2 * LANES)
        cols_gate = pl.ds(pl.multiple_of(chans + at, 2 * LANES), 2 * LANES)
        val = jnp.dot(normed[...], gb[:, :, cols].reshape(width, 2 * LANES), preferred_element_type=F32)
        gate = jnp.dot(
            normed[...], gb[:, :, cols_gate].reshape(width, 2 * LANES), preferred_element_type=F32
        )
        g = (val * jax.nn.sigmoid(gate)).astype(BF)
        gated[:, cols] = g
        pad[RIM:, cols] = g.astype(F32)
        return carry

    lax.fori_loop(0, chans // (2 * LANES), glu_step, 0)

    rim_copy = pltpu.make_async_remote_copy(
        gated.at[pl.ds(rows - RIM, RIM), :],
        rim,
        rims.at[0],
        rims.at[1],
        device_id=right,
        device_id_type=MESH,
    )

    @pl.when(has_right)
    def _():
        rim_copy.start()

    if n > 2:
        kv_take(2)
        attend_back(2)
    advance(len(items))

    @pl.when(has_left)
    def _():
        rim_copy.wait_recv()
        pad[:RIM, :] = rim[...].astype(F32)

    @pl.when(s == 0)
    def _():
        pad[:RIM, :] = jnp.zeros((RIM, chans), F32)

    taps = taps_r.shape[0]
    shift = RIM - (taps - 1)
    tile = min(128, rows)

    def conv_step(i, carry):
        cols = pl.ds(pl.multiple_of(i * LANES, LANES), LANES)
        for r in range(0, rows, tile):
            total = jnp.zeros((tile, LANES), F32)
            for j in range(taps):
                total = total + taps_r[j : j + 1, cols].astype(F32) * pad[
                    r + shift + j : r + shift + j + tile, cols
                ]
            conv[r : r + tile, cols] = total.astype(BF).astype(F32)
        return carry

    lax.fori_loop(0, chans // LANES, conv_step, 0)
    cv = conv[...]
    sq_own[...] = jnp.broadcast_to(jnp.sum(cv * cv, axis=-1, keepdims=True), (rows, LANES))
    sq_copy = pltpu.make_async_remote_copy(
        sq_own, sq_in, sqs.at[0], sqs.at[1], device_id=mate, device_id_type=MESH
    )
    sq_copy.start()

    for k in range(3, n):
        kv_take(k)
        attend_back(k)

    def head_rows(i, carry):
        at = pl.multiple_of(i * tile, tile)
        ids = lax.broadcasted_iota(jnp.int32, (tile, LANES), 1)
        logs = jnp.zeros((tile, LANES), F32)
        for h in range(heads):
            a0 = acc[h, pl.ds(at, tile), :]
            a1 = acc[h, pl.ds(pl.multiple_of(rows + at, tile), tile), :]
            t0, t1 = a0[:, VDIM:], a1[:, VDIM:]
            diff = a0[:, :VDIM] / t0 - lam_r[h] * (a1[:, :VDIM] / t1)
            out = (
                diff
                * lax.rsqrt(jnp.mean(diff * diff, axis=-1, keepdims=True) + EPS)
                * hgain_r[...].astype(F32)
            )
            both[pl.ds(at, tile), h * VDIM : (h + 1) * VDIM] = out.astype(BF)
            logs = jnp.where(ids == 2 * h, jnp.log(t0), logs)
            logs = jnp.where(ids == 2 * h + 1, jnp.log(t1), logs)
        log_r[:, pl.ds(at, tile)] = logs.T[: 2 * heads, :]
        return carry

    lax.fori_loop(0, rows // tile, head_rows, 0)
    stage2(*items[-1])

    sq_copy.wait()
    inv = lax.rsqrt((sq_own[:, :1] + sq_in[:, :1]) / conv_total + EPS)
    cgain = cgain_r[pl.ds(pl.multiple_of(t * chans, LANES), chans)].reshape(1, chans).astype(F32)
    both[:, att_rows:] = jax.nn.silu(conv[...] * inv * cgain).astype(BF)

    def pcopy(o):
        return pltpu.make_async_remote_copy(
            part_out.at[o], part_in.at[o], ps.at[o], pr.at[o], device_id=mate, device_id_type=MESH
        )

    ocols = gc.shape[2]
    mine = pl.ds(pl.multiple_of(t * half, half), half)
    other = pl.ds(pl.multiple_of((1 - t) * half, half), half)

    def out_block(o, _):
        part_out[o] = jnp.dot(both[other, :], gc[o], preferred_element_type=F32).astype(BF)
        pcopy(o).start()
        own = jnp.dot(both[mine, :], gc[o], preferred_element_type=F32)
        keep[o] = own

    out_block(s, None)
    for k in range(1, n):
        stage3(3, k)
        sides(k, out_block)

    def finish(o, carry):
        pcopy(o).wait_recv()
        pcopy(o).wait_send()
        mixed_r[:, pl.ds(pl.multiple_of(o * ocols, ocols), ocols)] = (
            keep[o] + part_in[o].astype(F32)
        ).astype(BF)
        return carry

    lax.fori_loop(0, n, finish, 0)

    for g in range(4):
        drain(g)

    @pl.when(has_right)
    def _():
        rim_copy.wait_send()
        for c in kvcopy(s):
            c.wait_send()

    for k in range(1, n):

        @pl.when((s >= k) & has_right)
        def _():
            for c in kvcopy(s - k):
                c.wait_send()


def body(n, conv_total, tokens, norm_gain, w_query, w_key, w_value, w_gv, w_gg, taps, cgain, hgain, lam, w_out):
    rows, width = tokens.shape
    heads = lam.shape[0]
    chans = w_gv.shape[1]
    qcols = w_query.shape[1]
    wrows = w_query.shape[0]
    ocols = w_out.shape[1]
    half = rows // 2
    any_ = pl.BlockSpec(memory_space=pl.ANY)
    vm = pl.BlockSpec(memory_space=pltpu.VMEM)
    sm = pl.BlockSpec(memory_space=pltpu.SMEM)
    dma = pltpu.SemaphoreType.DMA
    v = pltpu.VMEM
    mixed, logs = pl.pallas_call(
        functools.partial(kernel, n, conv_total),
        out_shape=(
            jax.ShapeDtypeStruct((half, width), BF),
            jax.ShapeDtypeStruct((2 * heads, rows), F32),
        ),
        in_specs=[any_, vm, any_, any_, any_, any_, any_, vm, vm, vm, sm, any_],
        out_specs=(vm, vm),
        scratch_shapes=[
            v((rows, width), BF),
            v((rows, width), BF),
            v((n, wrows, 2 * LANES), BF),
            v((n, wrows, qcols), BF),
            v((n, wrows, 2 * chans), BF),
            v((n, heads * VDIM + chans, ocols), BF),
            v((heads, 2 * rows, LANES), BF),
            v((n, rows, LANES), BF),
            v((n, rows, LANES), BF),
            v((heads, 2 * rows, 2 * VDIM), F32),
            v((rows, chans), BF),
            v((RIM, chans), BF),
            v((rows + RIM, chans), F32),
            v((rows, chans), F32),
            v((rows, LANES), F32),
            v((rows, LANES), F32),
            v((rows, heads * VDIM + chans), BF),
            v((n, half, ocols), BF),
            v((n, half, ocols), BF),
            v((n, half, ocols), F32),
            dma((8,)),
            dma((4, 2, n)),
            dma((4, n)),
            dma((4, n)),
            dma((4, n)),
            dma((4, n)),
            dma((4, n)),
            dma((4, n)),
            dma((4, n)),
            dma((4, n)),
            dma((4, n)),
            dma((2, n)),
            dma((2, n)),
            dma((2,)),
            dma((2,)),
            dma((n,)),
            dma((n,)),
        ],
        compiler_params=pltpu.CompilerParams(
            collective_id=0, has_side_effects=True, vmem_limit_bytes=60 * 1024 * 1024
        ),
    )(
        tokens,
        norm_gain,
        w_query,
        w_key,
        w_value,
        w_gv,
        w_gg,
        taps,
        cgain,
        hgain.reshape(1, -1),
        lam,
        w_out,
    )
    return mixed, logs.T


def solution(mesh):
    n = mesh.shape["sp"]

    def run(*args):
        return body(n, args[8].shape[0], *args)

    return jax.shard_map(
        run,
        mesh=mesh,
        in_specs=(
            P(("fs", "sp"), None),
            P(),
            P("sp", "tp"),
            P("sp", "tp"),
            P("sp", "tp"),
            P("sp", "tp"),
            P("sp", "tp"),
            P(None, "tp"),
            P(),
            P(),
            P("tp"),
            P(None, "sp"),
        ),
        out_specs=(P(("fs", "sp", "tp"), None), P(("fs", "sp"), "tp")),
        check_vma=False,
    )
```

```python
import functools
import math

import jax
import jax.numpy as jnp
from jax import lax
from jax.experimental import pallas as pl
from jax.experimental.pallas import tpu as pltpu
from jax.sharding import PartitionSpec as P

QK = 64
VDIM = 128
EPS = 1e-06
MESH = pl.DeviceIdType.MESH
BF = jnp.bfloat16
F32 = jnp.float32
LANES = 128
RIM = 32


def kernel(
    n,
    conv_total,
    tok_h,
    gain_r,
    wq_h,
    wk_h,
    wv_h,
    wgv_h,
    wgg_h,
    taps_r,
    cgain_r,
    hgain_r,
    lam_r,
    wo_h,
    mixed_r,
    log_r,
    tok,
    normed,
    gkv,
    gq,
    gb,
    gc,
    q2,
    kbuf,
    vbuf,
    acc,
    gated,
    rim,
    pad,
    conv,
    sq_own,
    sq_in,
    both,
    part_out,
    part_in,
    keep,
    loc,
    zs,
    zr,
    xs,
    xr,
    ys,
    yr,
    hxs,
    hxr,
    hys,
    hyr,
    kvs,
    kvr,
    rims,
    sqs,
    ps,
    pr,
):
    s = lax.axis_index("sp")
    f = lax.axis_index("fs")
    t = lax.axis_index("tp")
    fx = f + 1 - 2 * (f % 2)
    fy = (f + 2) % 4
    left = {"sp": s - 1, "fs": f, "tp": t}
    right = {"sp": s + 1, "fs": f, "tp": t}
    xdev = {"sp": s, "fs": fx, "tp": t}
    ydev = {"sp": s, "fs": fy, "tp": t}
    mate = {"sp": s, "fs": f, "tp": 1 - t}
    rows, width = tok.shape
    heads = lam_r.shape[0]
    chans = gated.shape[1]
    qcols = wq_h.shape[1]
    half = rows // 2
    groups = (gkv, gq, gb, gc)
    has_left = s > 0
    has_right = s < n - 1

    d_rows = wq_h.shape[0]
    att_rows = heads * VDIM
    locals_ = [
        (wk_h, gkv.at[s, :, pl.ds(0, LANES)]),
        (wv_h, gkv.at[s, :, pl.ds(LANES, LANES)]),
        (wq_h, gq.at[s]),
        (tok_h, tok),
        (wgv_h, gb.at[s, :, pl.ds(0, chans)]),
        (wgg_h, gb.at[s, :, pl.ds(chans, chans)]),
        (wo_h.at[pl.ds(t * att_rows, att_rows), :], gc.at[s, pl.ds(0, att_rows), :]),
        (
            wo_h.at[pl.ds(2 * att_rows + t * chans, chans), :],
            gc.at[s, pl.ds(att_rows, chans), :],
        ),
    ]
    copies = [pltpu.make_async_copy(a, b, loc.at[i]) for i, (a, b) in enumerate(locals_)]
    for c in copies:
        c.start()

    bar = pltpu.get_barrier_semaphore()
    for dev in (xdev, ydev, mate):
        pl.semaphore_signal(bar, 1, device_id=dev, device_id_type=MESH)

    @pl.when(has_left)
    def _():
        pl.semaphore_signal(bar, 1, device_id=left, device_id_type=MESH)

    @pl.when(has_right)
    def _():
        pl.semaphore_signal(bar, 1, device_id=right, device_id_type=MESH)

    pl.semaphore_wait(bar, 3 + jnp.where(has_left, 1, 0) + jnp.where(has_right, 1, 0))

    def chunk(g, o, q, part=None):
        buf = groups[g]
        size = buf.shape[1] // 4
        if part is None:
            return buf.at[o, pl.ds(pl.multiple_of(q * size, size), size), :]
        size = size // 2
        return buf.at[o, pl.ds(pl.multiple_of((q * 2 + part) * size, size), size), :]

    def zcopy(g, o, right_way):
        c = chunk(g, o, f)
        return pltpu.make_async_remote_copy(
            c,
            c,
            zs.at[g, 0 if right_way else 1, o],
            zr.at[g, o],
            device_id=right if right_way else left,
            device_id_type=MESH,
        )

    def xcopy(g, o, q):
        c = chunk(g, o, q)
        return pltpu.make_async_remote_copy(
            c, c, xs.at[g, o], xr.at[g, o], device_id=xdev, device_id_type=MESH
        )

    def ycopy(g, o, q):
        c = chunk(g, o, q)
        return pltpu.make_async_remote_copy(
            c, c, ys.at[g, o], yr.at[g, o], device_id=ydev, device_id_type=MESH
        )

    def hxcopy(g, o, q):
        c = chunk(g, o, q, 0)
        return pltpu.make_async_remote_copy(
            c, c, hxs.at[g, o], hxr.at[g, o], device_id=xdev, device_id_type=MESH
        )

    def hycopy(g, o, q):
        c = chunk(g, o, q, 1)
        return pltpu.make_async_remote_copy(
            c, c, hys.at[g, o], hyr.at[g, o], device_id=ydev, device_id_type=MESH
        )

    fd = 3 - f

    def sides(k, fn):
        @pl.when(s >= k)
        def _():
            fn(s - k, True)

        @pl.when(s + k < n)
        def _():
            fn(s + k, False)

    def own_send(g):
        @pl.when(has_right)
        def _():
            zcopy(g, s, True).start()

        @pl.when(has_left)
        def _():
            zcopy(g, s, False).start()

    def stage0(g, k):
        def go(o, right_way):
            zcopy(g, o, right_way).wait_recv()

            @pl.when(has_right if right_way else has_left)
            def _():
                zcopy(g, o, right_way).start()

        sides(k, go)

    def stage1(g, k):
        def go(o, right_way):
            xcopy(g, o, f).start()
            ycopy(g, o, f).start()

        sides(k, go)

    def stage2(g, k):
        def go(o, right_way):
            xcopy(g, o, fx).wait_recv()
            hycopy(g, o, fx).start()
            ycopy(g, o, fy).wait_recv()
            hxcopy(g, o, fy).start()

        sides(k, go)

    def stage3(g, k):
        def go(o, right_way):
            hxcopy(g, o, fd).wait_recv()
            hycopy(g, o, fd).wait_recv()

        sides(k, go)

    def drain(g):
        own = zcopy(g, s, True)

        @pl.when(has_right)
        def _():
            own.wait_send()

        @pl.when(has_left)
        def _():
            zcopy(g, s, False).wait_send()

        for k in range(1, n):

            def go(o, right_way):
                xcopy(g, o, f).wait_send()
                ycopy(g, o, f).wait_send()
                hycopy(g, o, fx).wait_send()
                hxcopy(g, o, fy).wait_send()

                @pl.when(has_right if right_way else has_left)
                def _():
                    zcopy(g, o, right_way).wait_send()

            sides(k, go)

    def kvcopy(o):
        return [
            pltpu.make_async_remote_copy(
                b.at[o], b.at[o], kvs.at[i, o], kvr.at[i, o], device_id=right, device_id_type=MESH
            )
            for i, b in enumerate((kbuf, vbuf))
        ]

    def kv_take(k):
        @pl.when(s >= k)
        def _():
            for c in kvcopy(s - k):
                c.wait_recv()

            @pl.when(has_right)
            def _():
                for c in kvcopy(s - k):
                    c.start()

    tall = min(256, rows)
    per_head = 2 * rows // tall

    def attend(o, diagonal):
        vx = jnp.concatenate([vbuf[o], jnp.ones((rows, VDIM), BF)], axis=1)
        kx = kbuf[o]

        def step(i, carry):
            h = i // per_head
            at = pl.multiple_of((i % per_head) * tall, tall)
            score = lax.dot_general(
                q2[h, pl.ds(at, tall), :],
                kx,
                (((1,), (1,)), ((), ())),
                preferred_element_type=F32,
            )
            w = jnp.exp2(score * (QK**-0.5 * math.log2(math.e)))
            if diagonal:
                pos = (at % rows) + lax.broadcasted_iota(jnp.int32, w.shape, 0)
                w = jnp.where(lax.broadcasted_iota(jnp.int32, w.shape, 1) <= pos, w, 0.0)
            pv = jnp.dot(w.astype(BF), vx, preferred_element_type=F32)
            if diagonal:
                acc[h, pl.ds(at, tall), :] = pv
            else:
                acc[h, pl.ds(at, tall), :] += pv
            return carry

        lax.fori_loop(0, heads * per_head, step, 0, unroll=2)

    def attend_back(k):
        @pl.when(s >= k)
        def _():
            attend(s - k, False)

    items = [(g, k) for g in range(4) for k in range(1, n)]
    per = n - 1
    state = {"at": 0, "in": 0}

    def advance(to):
        to = min(to, len(items))
        for i in range(state["at"], to):
            if state["in"] == i:
                stage0(*items[i])
                state["in"] += 1
            stage1(*items[i])
            if i == per:
                own_send(2)
            if i == 2 * per:
                own_send(3)
            if i > 0:
                stage2(*items[i - 1])
            if i >= 2 * per and i + 1 < len(items):
                stage0(*items[i + 1])
                state["in"] += 1
        state["at"] = max(state["at"], to)

    def arrived(g):
        for k in range(1, n):
            stage3(g, k)

    for c in copies[:2]:
        c.wait()
    own_send(0)
    copies[2].wait()
    own_send(1)
    copies[3].wait()

    gain = gain_r[...].reshape(1, width).astype(F32)

    def norm_step(i, carry):
        at = pl.ds(pl.multiple_of(i * 32, 32), 32)
        x = tok[at, :].astype(F32)
        r = lax.rsqrt(jnp.mean(x * x, axis=-1, keepdims=True) + EPS)
        normed[at, :] = (x * r * gain).astype(BF)
        return carry

    def norm_rows(lo, hi):
        lax.fori_loop(lo, hi, norm_step, 0)

    steps = rows // 32
    norm_rows(0, steps // 2)
    advance(1)
    norm_rows(steps // 2, steps)
    for c in copies[4:]:
        c.wait()
    advance(per + 2)
    arrived(0)

    lane = lax.broadcasted_iota(jnp.int32, (rows, LANES), 1)

    kv = jnp.dot(
        normed[...],
        gkv[...].reshape(width, 2 * LANES),
        preferred_element_type=F32,
    ).astype(BF)
    kbuf[s] = kv[:, :LANES]
    vbuf[s] = kv[:, LANES:]

    @pl.when(has_right)
    def _():
        for c in kvcopy(s):
            c.start()

    advance(2 * per + 2)
    arrived(1)

    def q_step(h, carry):
        cols = pl.ds(pl.multiple_of(h * 2 * LANES, 2 * LANES), 2 * LANES)
        q = jnp.dot(normed[...], gq[:, :, cols].reshape(width, 2 * LANES), preferred_element_type=F32)
        for e in range(2):
            one = q[:, e * LANES : (e + 1) * LANES]
            q2[2 * h + e, :rows, :] = jnp.where(lane < QK, one, 0.0).astype(BF)
            q2[2 * h + e, rows:, :] = jnp.where(lane >= QK, one, 0.0).astype(BF)
        return carry

    lax.fori_loop(0, heads // 2, q_step, 0)

    attend(s, True)
    advance(3 * per + 1)
    kv_take(1)
    attend_back(1)
    advance(3 * per + 2)
    arrived(2)

    def glu_step(i, carry):
        at = pl.multiple_of(i * 2 * LANES, 2 * LANES)
        cols = pl.ds(at, 2 * LANES)
        cols_gate = pl.ds(pl.multiple_of(chans + at, 2 * LANES), 2 * LANES)
        val = jnp.dot(normed[...], gb[:, :, cols].reshape(width, 2 * LANES), preferred_element_type=F32)
        gate = jnp.dot(
            normed[...], gb[:, :, cols_gate].reshape(width, 2 * LANES), preferred_element_type=F32
        )
        g = (val * jax.nn.sigmoid(gate)).astype(BF)
        gated[:, cols] = g
        pad[RIM:, cols] = g.astype(F32)
        return carry

    lax.fori_loop(0, chans // (2 * LANES), glu_step, 0)

    rim_copy = pltpu.make_async_remote_copy(
        gated.at[pl.ds(rows - RIM, RIM), :],
        rim,
        rims.at[0],
        rims.at[1],
        device_id=right,
        device_id_type=MESH,
    )

    @pl.when(has_right)
    def _():
        rim_copy.start()

    if n > 2:
        kv_take(2)
        attend_back(2)
    advance(len(items))

    @pl.when(has_left)
    def _():
        rim_copy.wait_recv()
        pad[:RIM, :] = rim[...].astype(F32)

    @pl.when(s == 0)
    def _():
        pad[:RIM, :] = jnp.zeros((RIM, chans), F32)

    taps = taps_r.shape[0]
    shift = RIM - (taps - 1)
    tile = min(128, rows)

    def conv_step(i, carry):
        cols = pl.ds(pl.multiple_of(i * LANES, LANES), LANES)
        for r in range(0, rows, tile):
            total = jnp.zeros((tile, LANES), F32)
            for j in range(taps):
                total = total + taps_r[j : j + 1, cols].astype(F32) * pad[
                    r + shift + j : r + shift + j + tile, cols
                ]
            conv[r : r + tile, cols] = total.astype(BF).astype(F32)
        return carry

    lax.fori_loop(0, chans // LANES, conv_step, 0)
    cv = conv[...]
    sq_own[...] = jnp.broadcast_to(jnp.sum(cv * cv, axis=-1, keepdims=True), (rows, LANES))
    sq_copy = pltpu.make_async_remote_copy(
        sq_own, sq_in, sqs.at[0], sqs.at[1], device_id=mate, device_id_type=MESH
    )
    sq_copy.start()

    for k in range(3, n):
        kv_take(k)
        attend_back(k)

    def head_rows(i, carry):
        at = pl.multiple_of(i * tile, tile)
        ids = lax.broadcasted_iota(jnp.int32, (tile, LANES), 1)
        logs = jnp.zeros((tile, LANES), F32)
        for h in range(heads):
            a0 = acc[h, pl.ds(at, tile), :]
            a1 = acc[h, pl.ds(pl.multiple_of(rows + at, tile), tile), :]
            t0, t1 = a0[:, VDIM:], a1[:, VDIM:]
            diff = a0[:, :VDIM] / t0 - lam_r[h] * (a1[:, :VDIM] / t1)
            out = (
                diff
                * lax.rsqrt(jnp.mean(diff * diff, axis=-1, keepdims=True) + EPS)
                * hgain_r[...].astype(F32)
            )
            both[pl.ds(at, tile), h * VDIM : (h + 1) * VDIM] = out.astype(BF)
            logs = jnp.where(ids == 2 * h, jnp.log(t0), logs)
            logs = jnp.where(ids == 2 * h + 1, jnp.log(t1), logs)
        log_r[:, pl.ds(at, tile)] = logs.T[: 2 * heads, :]
        return carry

    lax.fori_loop(0, rows // tile, head_rows, 0)
    stage2(*items[-1])

    sq_copy.wait()
    inv = lax.rsqrt((sq_own[:, :1] + sq_in[:, :1]) / conv_total + EPS)
    cgain = cgain_r[pl.ds(pl.multiple_of(t * chans, LANES), chans)].reshape(1, chans).astype(F32)
    both[:, att_rows:] = jax.nn.silu(conv[...] * inv * cgain).astype(BF)

    def pcopy(o):
        return pltpu.make_async_remote_copy(
            part_out.at[o], part_in.at[o], ps.at[o], pr.at[o], device_id=mate, device_id_type=MESH
        )

    ocols = gc.shape[2]
    mine = pl.ds(pl.multiple_of(t * half, half), half)
    other = pl.ds(pl.multiple_of((1 - t) * half, half), half)

    def out_block(o, _):
        part_out[o] = jnp.dot(both[other, :], gc[o], preferred_element_type=F32).astype(BF)
        pcopy(o).start()
        own = jnp.dot(both[mine, :], gc[o], preferred_element_type=F32)
        keep[o] = own

    out_block(s, None)
    for k in range(1, n):
        stage3(3, k)
        sides(k, out_block)

    def finish(o, carry):
        pcopy(o).wait_recv()
        pcopy(o).wait_send()
        mixed_r[:, pl.ds(pl.multiple_of(o * ocols, ocols), ocols)] = (
            keep[o] + part_in[o].astype(F32)
        ).astype(BF)
        return carry

    lax.fori_loop(0, n, finish, 0)

    for g in range(4):
        drain(g)

    @pl.when(has_right)
    def _():
        rim_copy.wait_send()
        for c in kvcopy(s):
            c.wait_send()

    for k in range(1, n):

        @pl.when((s >= k) & has_right)
        def _():
            for c in kvcopy(s - k):
                c.wait_send()


def body(n, conv_total, tokens, norm_gain, w_query, w_key, w_value, w_gv, w_gg, taps, cgain, hgain, lam, w_out):
    rows, width = tokens.shape
    heads = lam.shape[0]
    chans = w_gv.shape[1]
    qcols = w_query.shape[1]
    wrows = w_query.shape[0]
    ocols = w_out.shape[1]
    half = rows // 2
    any_ = pl.BlockSpec(memory_space=pl.ANY)
    vm = pl.BlockSpec(memory_space=pltpu.VMEM)
    sm = pl.BlockSpec(memory_space=pltpu.SMEM)
    dma = pltpu.SemaphoreType.DMA
    v = pltpu.VMEM
    mixed, logs = pl.pallas_call(
        functools.partial(kernel, n, conv_total),
        out_shape=(
            jax.ShapeDtypeStruct((half, width), BF),
            jax.ShapeDtypeStruct((2 * heads, rows), F32),
        ),
        in_specs=[any_, vm, any_, any_, any_, any_, any_, vm, vm, vm, sm, any_],
        out_specs=(vm, vm),
        scratch_shapes=[
            v((rows, width), BF),
            v((rows, width), BF),
            v((n, wrows, 2 * LANES), BF),
            v((n, wrows, qcols), BF),
            v((n, wrows, 2 * chans), BF),
            v((n, heads * VDIM + chans, ocols), BF),
            v((heads, 2 * rows, LANES), BF),
            v((n, rows, LANES), BF),
            v((n, rows, LANES), BF),
            v((heads, 2 * rows, 2 * VDIM), F32),
            v((rows, chans), BF),
            v((RIM, chans), BF),
            v((rows + RIM, chans), F32),
            v((rows, chans), F32),
            v((rows, LANES), F32),
            v((rows, LANES), F32),
            v((rows, heads * VDIM + chans), BF),
            v((n, half, ocols), BF),
            v((n, half, ocols), BF),
            v((n, half, ocols), F32),
            dma((8,)),
            dma((4, 2, n)),
            dma((4, n)),
            dma((4, n)),
            dma((4, n)),
            dma((4, n)),
            dma((4, n)),
            dma((4, n)),
            dma((4, n)),
            dma((4, n)),
            dma((4, n)),
            dma((2, n)),
            dma((2, n)),
            dma((2,)),
            dma((2,)),
            dma((n,)),
            dma((n,)),
        ],
        compiler_params=pltpu.CompilerParams(
            collective_id=0, has_side_effects=True, vmem_limit_bytes=60 * 1024 * 1024
        ),
    )(
        tokens,
        norm_gain,
        w_query,
        w_key,
        w_value,
        w_gv,
        w_gg,
        taps,
        cgain,
        hgain.reshape(1, -1),
        lam,
        w_out,
    )
    return mixed, logs.T


def solution(mesh):
    n = mesh.shape["sp"]

    def run(*args):
        return body(n, args[8].shape[0], *args)

    return jax.shard_map(
        run,
        mesh=mesh,
        in_specs=(
            P(("fs", "sp"), None),
            P(),
            P("sp", "tp"),
            P("sp", "tp"),
            P("sp", "tp"),
            P("sp", "tp"),
            P("sp", "tp"),
            P(None, "tp"),
            P(),
            P(),
            P("tp"),
            P(None, "sp"),
        ),
        out_specs=(P(("fs", "sp", "tp"), None), P(("fs", "sp"), "tp")),
        check_vma=False,
    )
```
